256 devices in a mesh: grp: 2 (over y), ep: 32 (over z, core), tp: 4 (over x).
Axes of the slice: x: 4, y: 2, z: 16, core: 2. Of those that a mesh axis runs over, the one named last changes fastest.
The devices are a block of a 4x16x16 slice.
Arguments:
- outer_gate: bfloat16 [32768, 1024], P(('grp', 'ep'), 'tp'), parts along dimension 0, may hold values from -6 to 6
- inner_gate: bfloat16 [32768, 1024], P(('grp', 'ep'), 'tp'), parts along dimension 0, may hold values from -6 to 6
- conv_input: bfloat16 [32768, 1024], P(('grp', 'ep'), 'tp'), parts along dimension 0, may hold values from -6 to 6
- conv_taps: float32 [3, 1024], P(None, 'tp'), may hold values from -3.5 to 3.5
- mixer_weight: bfloat16 [1024, 2048], P('tp'), may hold values from -0.1875 to 0.1875
- expert_input: bfloat16 [32768, 2048], P(('grp', 'ep', 'tp')), parts along dimension 0, may hold values from -6 to 6
- norm_gain: float32 [2048], replicated, may hold values from 0.1 to 1.9
- expert_ids: int32 [32768, 2], P(('grp', 'ep', 'tp')), parts along dimension 0, may hold values from 0 to 31, all different within a row; in each aligned block of 128 rows (0 to 127, 128 to 255, ...) at most 10 rows name the same one
- route_weight: float32 [32768, 2], P(('grp', 'ep', 'tp')), parts along dimension 0, may hold values from 0.25 to 1
- gate_weight: bfloat16 [32, 2048, 3072], P('ep', None, 'tp'), may hold values from -0.125 to 0.125
- up_weight: bfloat16 [32, 2048, 3072], P('ep', None, 'tp'), may hold values from -0.125 to 0.125
- down_weight: bfloat16 [32, 3072, 2048], P('ep', 'tp'), may hold values from -0.109375 to 0.109375
Outputs:
- mixer_output: bfloat16 [32768, 2048], P(('grp', 'ep', 'tp')), parts along dimension 0
- expert_output: bfloat16 [32768, 2048], P(('grp', 'ep', 'tp')), parts along dimension 0
The draws below stay inside these ranges and needn't reach their ends.
There are 2 independent parts, one for each index of `grp`. The reference program is written for one: setup_inputs(seed, part) draws one part's arguments, and reference() takes and returns one part's arrays. A program takes and returns all parts, laid end to end along the dimension named above; an argument that names none is the same for every part. Nothing has to cross between parts.
Inputs may be any that keep to these rules, and one draw needn't show every extreme that they name: `expert_ids`: each row names 2 different experts. Among the rows of one device no expert is named more than 10 times, a bound that some block reaches.
All inputs are finite; a program needn't handle non-finite values.
Results may differ from the reference program's by a relative error of at most 0.011.
Values may be sent and summed in bfloat16 or wider, within the bound.
A program may use at most 128 MiB of HBM per device.

```python
import math
import jax
import jax.numpy as jnp
import numpy as np
from jax import lax

D = 2048
CONV_W = 1024
TAPS = 3
FF_E = 3072
TOP = 2
TOK_DEV = 128
EXPERTS = 32
CAP = 10
TOKENS = 16384
N_EP = 32
N_TP = 4


def level_of(key, shape, cuts, low, largest):
    gain = 1.0
    for dim, parts in cuts:
        heights = jax.random.uniform(jax.random.fold_in(jax.random.fold_in(key, 6), dim), (parts,), jnp.float32, low / len(cuts), largest / len(cuts))
        gain = gain * jnp.repeat(jnp.exp(heights), shape[dim] // parts).reshape((-1,) + (1,) * (len(shape) - 1 - dim))
    return gain


def deal_out(key, own, number, rows, number_of, top, limit, slope):
    ranking = jax.random.permutation(key, number_of)
    packed, common = shares(number_of, rows * top, limit, slope, True), shares(number_of, rows * top, limit, slope, False)
    places = jnp.arange(number_of)

    def named(lengths, rotation):
        used = int((lengths > 0).sum())
        fixed = max(1, used // 4)
        moved = fixed + (places - fixed + rotation * (used - fixed)) % max(1, number_of - fixed)
        return jnp.zeros((number_of,), jnp.int32).at[ranking[jnp.where(places < fixed, places, moved)]].set(jnp.asarray(lengths, jnp.int32))

    lengths = jnp.where(number % 4 == 0, named(packed, number // 4), named(common, number - number // 4 - 1))
    mixed = jax.random.permutation(jax.random.fold_in(own, 3), number_of)
    source_of, taker = mixed[0:number_of // 2 * 2:2], mixed[1:number_of // 2 * 2:2]
    margin = jnp.minimum(lengths[source_of] - 1, limit - lengths[taker]) // 2
    margin = jnp.where((source_of == ranking[0]) | (taker == ranking[0]) | (lengths[taker] == 0), 0, jnp.maximum(margin, 0))
    moved = jax.random.randint(jax.random.fold_in(own, 4), (number_of // 2,), 0, 1 << 20) % (margin + 1)
    lengths = lengths.at[source_of].add(-moved).at[taker].add(moved)
    members = jnp.searchsorted(jnp.cumsum(lengths), jnp.arange(rows * top), side="right").astype(jnp.int32)
    table = members.reshape(top, rows).T
    table = table[jax.random.permutation(jax.random.fold_in(own, 1), rows)]
    rotation = jax.random.randint(jax.random.fold_in(own, 2), (rows, 1), 0, top)
    return jnp.take_along_axis(table, (jnp.arange(top)[None, :] + rotation) % top, axis=1)


def shares(number_of, total, reach, skew, full):
    portions = [(1 << 20) // math.isqrt(rank ** skew) + 1 for rank in range(1, number_of + 1)]
    largest = reach if full else min(reach, max(-(-total // number_of), total * portions[0] // sum(portions)))
    least = 1 if total - largest >= number_of - 1 else 0
    given, rest = [largest] + [least] * (number_of - 1), total - largest - least * (number_of - 1)
    while rest > 0:
        candidates = [i for i in range(1, number_of) if given[i] < largest] or [i for i in range(1, number_of) if given[i] < reach]
        mass, budget = sum([portions[i] for i in candidates]), rest
        for i in candidates:
            extra = min(reach - given[i], max(1, budget * portions[i] // mass), rest)
            given[i] = given[i] + extra
            rest = rest - extra
    return np.array(given)


def normal_values(stream_key, extent, width, most, split=(), kind=jnp.bfloat16):
    entries = width * jax.random.normal(stream_key, extent, jnp.float32)
    if split:
        entries = entries * level_of(stream_key, extent, split, -0.22, 0.18)
    return jnp.clip(entries, -most, most).astype(kind)


def setup_inputs(seed: int = 0, part: int = 0) -> dict:
    key_of = jax.random.split(jax.random.key(seed), 13)
    part_keys = jax.random.split(jax.random.fold_in(key_of[12], part), 13)
    outer_gate = normal_values(part_keys[0], (TOKENS, CONV_W), 1.0, 6.0, ((0, 32), (1, 4)))
    inner_gate = normal_values(part_keys[1], (TOKENS, CONV_W), 1.0, 6.0, ((0, 32), (1, 4)))
    conv_input = normal_values(part_keys[2], (TOKENS, CONV_W), 1.0, 6.0, ((0, 32), (1, 4)))
    conv_taps = normal_values(key_of[3], (TAPS, CONV_W), TAPS ** -0.5, 3.5, ((1, 4),), jnp.float32)
    mixer_weight = normal_values(key_of[4], (CONV_W, D), CONV_W ** -0.5, 0.1875, ((0, 4),))
    expert_input = normal_values(part_keys[5], (TOKENS, D), 1.0, 6.0, ((0, 128),))
    norm_gain = jnp.clip(1.0 + 0.18 * jax.random.normal(key_of[6], (D,), jnp.float32), 0.1, 1.9)
    expert_ids_keys = jax.random.split(jax.random.fold_in(part_keys[7], 1), TOKENS // TOK_DEV)
    expert_ids_turns = jax.random.permutation(jax.random.fold_in(part_keys[7], 3), TOKENS // TOK_DEV)
    expert_ids = jax.vmap(lambda own, number: deal_out(jax.random.fold_in(part_keys[7], 2), own, number, TOK_DEV, EXPERTS, TOP, CAP, 1))(expert_ids_keys, expert_ids_turns).reshape((TOKENS, TOP))
    route_weight = jnp.clip(jnp.exp(math.log(1.0) - 1.3862944 * jax.random.uniform(part_keys[8], (TOKENS, TOP), jnp.float32) ** level_of(part_keys[8], (TOKENS, TOP), ((0, 128),), -0.2, 0.2)), 0.25, 1.0)
    gate_weight = normal_values(key_of[9], (EXPERTS, D, FF_E), D ** -0.5, 0.125, ((0, 32), (2, 4)))
    up_weight = normal_values(key_of[10], (EXPERTS, D, FF_E), D ** -0.5, 0.125, ((0, 32), (2, 4)))
    down_weight = normal_values(key_of[11], (EXPERTS, FF_E, D), FF_E ** -0.5, 0.109375, ((0, 32), (1, 4)))
    return {"outer_gate": outer_gate, "inner_gate": inner_gate, "conv_input": conv_input, "conv_taps": conv_taps, "mixer_weight": mixer_weight, "expert_input": expert_input, "norm_gain": norm_gain, "expert_ids": expert_ids, "route_weight": route_weight, "gate_weight": gate_weight, "up_weight": up_weight, "down_weight": down_weight}


epsilon = 1e-06

def rounded_sum(operand, weights, pieces):
    slice_width = operand.shape[1] // pieces
    summed = jnp.zeros((operand.shape[0], weights.shape[1]), jnp.float32)
    for piece_index in range(pieces):
        lower = piece_index * slice_width
        partial_value = jnp.dot(operand[:, lower:lower + slice_width], weights[lower:lower + slice_width], preferred_element_type=jnp.float32)
        summed = summed + lax.optimization_barrier(partial_value.astype(jnp.bfloat16)).astype(jnp.float32)
    return summed.astype(jnp.bfloat16)

def reference(outer_gate, inner_gate, conv_input, conv_taps, mixer_weight, expert_input, norm_gain, expert_ids, route_weight, gate_weight, up_weight, down_weight):
    gated_rows = inner_gate.astype(jnp.float32) * conv_input.astype(jnp.float32)
    length = gated_rows.shape[0]
    padded = jnp.pad(gated_rows, ((TAPS - 1, 0), (0, 0)))
    convolved = jnp.zeros_like(gated_rows)
    for tap_index in range(TAPS):
        convolved = convolved + conv_taps[tap_index] * padded[tap_index:tap_index + length]
    mixed = (outer_gate.astype(jnp.float32) * convolved).astype(jnp.bfloat16)
    mixer_output = rounded_sum(mixed, mixer_weight, N_TP)
    inputs = expert_input.astype(jnp.float32)
    normed = (inputs * lax.rsqrt(lax.optimization_barrier(jnp.mean(inputs * inputs, axis=1, keepdims=True)) + epsilon) * norm_gain).astype(jnp.bfloat16)
    flat_ids = expert_ids.reshape(-1)
    flat_weights = route_weight.reshape(-1)
    most_rows = N_EP * N_TP * CAP

    def one_expert(expert):
        chosen = flat_ids == expert
        picked = jnp.nonzero(chosen, size=most_rows, fill_value=0)[0].astype(jnp.int32)
        valid = jnp.arange(most_rows, dtype=jnp.int32) < jnp.sum(chosen.astype(jnp.int32))
        owners = (picked // TOP).astype(jnp.int32)
        token_rows = normed[owners]
        gate_value = jnp.dot(token_rows, gate_weight[expert], preferred_element_type=jnp.float32)
        up_value = jnp.dot(token_rows, up_weight[expert], preferred_element_type=jnp.float32)
        hidden = (jax.nn.silu(gate_value) * up_value).astype(jnp.bfloat16)
        answer = rounded_sum(hidden, down_weight[expert], N_TP)
        pair_weight = jnp.where(valid, flat_weights[picked], jnp.zeros_like(flat_weights[picked]))
        return (owners, answer.astype(jnp.float32) * pair_weight[:, None])
    owners, contributions = lax.map(one_expert, jnp.arange(EXPERTS, dtype=jnp.int32))
    summed = jax.ops.segment_sum(contributions.reshape(-1, D), owners.reshape(-1), num_segments=TOKENS)
    expert_output = summed.astype(jnp.bfloat16)
    return (mixer_output, expert_output)
```

```python
import functools

import jax
import jax.numpy as jnp
from jax import lax
from jax.experimental import pallas as pl
from jax.experimental.pallas import tpu as pltpu
from jax.sharding import PartitionSpec as P

TAPS = 3
CORES = 2
LANES = 128
EPSILON = 1e-06
MESH = pl.DeviceIdType.MESH
F32 = jnp.float32
BF16 = jnp.bfloat16


def remote(source, target, send, recv, where):
    return pltpu.make_async_remote_copy(
        src_ref=source,
        dst_ref=target,
        send_sem=send,
        recv_sem=recv,
        device_id=where,
        device_id_type=MESH,
    )


def dot(a, b):
    return jnp.dot(a, b, preferred_element_type=F32)


def kernel(
    n_ep,
    n_tp,
    cap,
    ids_ref,
    route_ref,
    tokens_ref,
    gain_ref,
    taps_ref,
    outer_hbm,
    inner_hbm,
    conv_hbm,
    mixw_hbm,
    gate_hbm,
    up_hbm,
    down_hbm,
    mixer_ref,
    expert_ref,
    outer,
    inner,
    conv,
    mixw,
    gate_w,
    up_w,
    down_w,
    normed,
    picks,
    wide,
    outgoing,
    gathered,
    rows_f,
    rows_b,
    hidden,
    partial,
    first_in,
    second_in,
    combined,
    summed,
    returned,
    answers,
    tail_out,
    tail_in,
    gated,
    mix_partial,
    mix_first,
    mix_second,
    mix_combined,
    load_sem,
    halo_send,
    halo_recv,
    z_send,
    z_recv,
    gather_send,
    gather_recv,
    relay_send,
    relay_recv,
    first_send,
    first_recv,
    direct_send,
    comb_send,
    second_recv,
    back_send,
    back_recv,
    mix_send,
    mix_first_recv,
    mix_second_recv,
):
    n_z = n_ep // CORES
    groups = n_z // 2
    last = groups - 1
    count = 2 * n_z
    tokens, width = tokens_ref.shape
    strips = width // LANES
    chunk = cap * strips
    slots = picks.shape[0]
    used = count * cap
    batch = 4 * 2 * CORES * cap

    me = lax.axis_index("ep")
    x = lax.axis_index("tp")
    z = me // CORES
    core = me % CORES
    right = {"tp": (x + 1) % n_tp}
    left = {"tp": (x + n_tp - 1) % n_tp}

    barrier = pltpu.get_barrier_semaphore()

    @pl.loop(1, n_ep)
    def _(k):
        pl.semaphore_signal(
            barrier, inc=1, device_id={"ep": (me + k) % n_ep}, device_id_type=MESH
        )

    pl.semaphore_signal(barrier, inc=1, device_id=right, device_id_type=MESH)
    pl.semaphore_signal(barrier, inc=1, device_id=left, device_id_type=MESH)

    loads = [
        pltpu.make_async_copy(source, target, load_sem.at[k])
        for k, (source, target) in enumerate(
            (
                (inner_hbm, inner),
                (conv_hbm, conv),
                (outer_hbm, outer),
                (mixw_hbm, mixw),
                (gate_hbm, gate_w),
                (up_hbm, up_w),
                (down_hbm, down_w),
            )
        )
    ]
    for load in loads:
        load.start()

    row = lax.broadcasted_iota(jnp.int32, (slots, tokens), 0)
    place = row * 0
    for k in range(1, slots // cap + 1):
        place = place + (row >= k * cap).astype(jnp.int32)
    slot = row - place * cap
    group_of = lax.shift_right_logical(place, 2)
    half_of = lax.shift_right_logical(place, 1) & 1
    offset = jnp.where(
        half_of == 0, group_of + 1, jnp.where(group_of == last, 0, n_z - 1 - group_of)
    )
    target_z = z - offset
    target_z = jnp.where(target_z < 0, target_z + n_z, target_z)
    expert = jnp.where(row < used, target_z * CORES + (place & 1), -1)
    first_named = ids_ref[0:1, :] == expert
    second_named = ids_ref[1:2, :] == expert
    named = jnp.where(first_named, 1.0, 0.0) + jnp.where(second_named, 1.0, 0.0)
    before = lax.broadcasted_iota(jnp.int32, (tokens, tokens), 0) < lax.broadcasted_iota(
        jnp.int32, (tokens, tokens), 1
    )
    rank = dot(named.astype(BF16), jnp.where(before, 1.0, 0.0).astype(BF16))
    chosen = jnp.where(rank == slot.astype(F32), named, 0.0)
    weight = jnp.where(first_named, route_ref[0:1, :], 0.0) + jnp.where(
        second_named, route_ref[1:2, :], 0.0
    )
    picks[...] = chosen * weight

    values = tokens_ref[...].astype(F32)
    mean = jnp.mean(values * values, axis=1, keepdims=True)
    normed[...] = (values * lax.rsqrt(mean + EPSILON) * gain_ref[...]).astype(BF16)
    one_hot = chosen[0:used, :].astype(BF16)
    for pair in range(strips // 2):
        rows = dot(one_hot, normed[:, 2 * pair * LANES : 2 * (pair + 1) * LANES])
        wide[pl.ds(2 * pair, used, stride=strips), :] = rows[:, :LANES]
        wide[pl.ds(2 * pair + 1, used, stride=strips), :] = rows[:, LANES:]

    @pl.loop(0, count)
    def _(k):
        outgoing[k] = wide[pl.ds(pl.multiple_of(k * chunk, 16), chunk), :].astype(BF16)

    loads[0].wait()
    loads[1].wait()
    length = inner.shape[0]
    gated[pl.ds(8, length), :] = inner[...].astype(F32) * conv[...].astype(F32)
    tail_out[...] = gated[pl.ds(length, 8), :]

    pl.semaphore_wait(barrier, n_ep + 1)

    def sent(g, half, to_core, from_slot):
        offset = g + 1 if half == 0 else n_z - 1 - g
        return remote(
            outgoing.at[from_slot],
            gathered.at[g, 0, half, core],
            z_send.at[0],
            z_recv.at[g, half],
            {"ep": ((z + n_z - offset) % n_z) * CORES + to_core},
        )

    @pl.loop(0, last)
    def _(g):
        for half in range(2):
            for to_core in range(CORES):
                sent(g, half, to_core, 4 * g + 2 * half + to_core).start()

    for to_core in range(CORES):
        sent(last, 0, to_core, 4 * last + to_core).start()
    other = 1 - core
    partner = {"ep": z * CORES + other}
    remote(
        outgoing.at[4 * last + 2 + other],
        gathered.at[last, 0, 1, core],
        z_send.at[0],
        z_recv.at[last, 1],
        partner,
    ).start()
    gathered[last, 0, 1, core] = outgoing[4 * last + 2 + core]
    halo = remote(
        tail_out, tail_in, halo_send.at[0], halo_recv.at[0], {"ep": (me + 1) % n_ep}
    )
    halo.start()

    for load in loads[2:4]:
        load.wait()
    halo.wait()
    gated[0:8, :] = jnp.where(me > 0, tail_in[...], 0.0)
    convolved = jnp.zeros((length, inner.shape[1]), F32)
    for tap in range(TAPS):
        convolved = convolved + taps_ref[tap : tap + 1, :] * gated[
            pl.ds(8 - (TAPS - 1) + tap, length), :
        ]
    inner[...] = (outer[...].astype(F32) * convolved).astype(BF16)
    half_rows = tokens // 2

    @pl.loop(0, n_tp * 2)
    def _(k):
        owner = (x + k // 2) % n_tp
        start = pl.multiple_of(owner * tokens + (k % 2) * half_rows, 16)
        mixed = inner[pl.ds(start, half_rows), :]
        for part in range(width // 512):
            columns = slice(part * 512, (part + 1) * 512)
            mix_partial[k // 2, k % 2, :, columns] = dot(mixed, mixw[:, columns]).astype(BF16)

    for load in loads[4:]:
        load.wait()

    def gather(g):
        block = gathered.at[g, 0, 0]
        remote(block, block, z_send.at[0], z_recv.at[g, 0], right).wait_recv()

        @pl.when(g < last)
        def _():
            block = gathered.at[g, 0, 1]
            remote(block, block, z_send.at[0], z_recv.at[g, 1], right).wait_recv()

        @pl.when(g == last)
        def _():
            block = gathered.at[g, 0, 1, 0]
            remote(block, block, z_send.at[0], z_recv.at[g, 1], right).wait_recv()

        remote(
            gathered.at[g, 0], gathered.at[g, 3], gather_send.at[0], gather_recv.at[g, 0], right
        ).start()
        remote(
            gathered.at[g, 0], gathered.at[g, 1], gather_send.at[1], gather_recv.at[g, 1], left
        ).start()

    def relay(g):
        remote(
            gathered.at[g, 0], gathered.at[g, 3], gather_send.at[0], gather_recv.at[g, 0], right
        ).wait_recv()
        remote(
            gathered.at[g, 3, 0], gathered.at[g, 2, 0], relay_send.at[0], relay_recv.at[g, 0], right
        ).start()
        remote(
            gathered.at[g, 0], gathered.at[g, 1], gather_send.at[1], gather_recv.at[g, 1], left
        ).wait_recv()
        remote(
            gathered.at[g, 1, 1], gathered.at[g, 2, 1], relay_send.at[1], relay_recv.at[g, 1], left
        ).start()

    def compute(g):
        remote(
            gathered.at[g, 3, 0], gathered.at[g, 2, 0], relay_send.at[0], relay_recv.at[g, 0], right
        ).wait_recv()
        remote(
            gathered.at[g, 1, 1], gathered.at[g, 2, 1], relay_send.at[1], relay_recv.at[g, 1], left
        ).wait_recv()
        for k in range(batch // cap):
            rows_f[k * chunk : (k + 1) * chunk, :] = gathered[
                g, k // 4, (k // 2) % 2, k % 2
            ].astype(F32)
        for strip in range(strips):
            rows_b[:, strip * LANES : (strip + 1) * LANES] = rows_f[
                pl.ds(strip, batch, stride=strips), :
            ].astype(BF16)
        units = hidden.shape[1]
        step = min(256, units)
        for part in range(units // step):
            columns = slice(part * step, (part + 1) * step)
            gate = dot(rows_b[...], gate_w[:, columns])
            up = dot(rows_b[...], up_w[:, columns])
            hidden[:, columns] = (gate / (1.0 + jnp.exp(-gate)) * up).astype(BF16)
        for pair in range(strips // 2):
            rows = dot(hidden[...], down_w[:, 2 * pair * LANES : 2 * (pair + 1) * LANES])
            rows_f[pl.ds(2 * pair, batch, stride=strips), :] = rows[:, :LANES]
            rows_f[pl.ds(2 * pair + 1, batch, stride=strips), :] = rows[:, LANES:]
        for k in range(batch // cap):
            partial[g, k // 4, (k // 2) % 2, k % 2] = rows_f[
                k * chunk : (k + 1) * chunk, :
            ].astype(BF16)
        remote(
            partial.at[g, 2, 0], first_in.at[g, 0], first_send.at[0], first_recv.at[g, 0], right
        ).start()
        remote(
            partial.at[g, 2, 1], first_in.at[g, 1], first_send.at[1], first_recv.at[g, 1], left
        ).start()
        remote(
            partial.at[g, 1, 1], second_in.at[g, 0, 1], direct_send.at[0], second_recv.at[g, 0], right
        ).start()
        remote(
            partial.at[g, 3, 0], second_in.at[g, 1, 0], direct_send.at[1], second_recv.at[g, 1], left
        ).start()

    def combine(g):
        for side, slot, where in ((0, 1, right), (1, 3, left)):
            remote(
                partial.at[g, 2, side], first_in.at[g, side], first_send.at[side],
                first_recv.at[g, side], where,
            ).wait_recv()
            combined[g, side] = (
                partial[g, slot, side].astype(F32) + first_in[g, side].astype(F32)
            ).astype(BF16)
            remote(
                combined.at[g, side], second_in.at[g, side, side], comb_send.at[side],
                second_recv.at[g, side], where,
            ).start()

    def back(g, half, to_core):
        offset = g + 1 if half == 0 else n_z - 1 - g
        return remote(
            summed.at[4 * g + 2 * half + to_core],
            returned.at[g, half, core],
            back_send.at[0],
            back_recv.at[g, half],
            {"ep": ((z + offset) % n_z) * CORES + to_core},
        )

    def give_back(g):
        for side, where in ((0, right), (1, left)):
            block = second_in.at[g, side]
            remote(block, block, comb_send.at[side], second_recv.at[g, side], where).wait_recv()
        for half in range(2):
            for from_core in range(CORES):
                summed[4 * g + 2 * half + from_core] = (
                    partial[g, 0, half, from_core].astype(F32)
                    + second_in[g, 0, half, from_core].astype(F32)
                    + second_in[g, 1, half, from_core].astype(F32)
                ).astype(BF16)

        @pl.when(g < last)
        def _():
            for half in range(2):
                for to_core in range(CORES):
                    back(g, half, to_core).start()

        @pl.when(g == last)
        def _():
            for to_core in range(CORES):
                back(last, 0, to_core).start()
            remote(
                summed.at[4 * last + 2 + other],
                returned.at[last, 1, core],
                back_send.at[0],
                back_recv.at[last, 1],
                partner,
            ).start()
            returned[last, 1, core] = summed[4 * last + 2 + core]

    def mix_start():
        remote(
            mix_partial.at[2, 0], mix_first.at[0], mix_send.at[0], mix_first_recv.at[0], right
        ).start()
        remote(
            mix_partial.at[2, 1], mix_first.at[1], mix_send.at[1], mix_first_recv.at[1], left
        ).start()
        remote(
            mix_partial.at[1, 1], mix_second.at[0, 1], mix_send.at[2], mix_second_recv.at[0, 1], right
        ).start()
        remote(
            mix_partial.at[3, 0], mix_second.at[1, 0], mix_send.at[3], mix_second_recv.at[1, 0], left
        ).start()

    def mix_combine():
        for side, slot, where in ((0, 1, right), (1, 3, left)):
            remote(
                mix_partial.at[2, side], mix_first.at[side], mix_send.at[side],
                mix_first_recv.at[side], where,
            ).wait_recv()
            mix_combined[side] = (
                mix_partial[slot, side].astype(F32) + mix_first[side].astype(F32)
            ).astype(BF16)
            remote(
                mix_combined.at[side], mix_second.at[side, side], mix_send.at[4 + side],
                mix_second_recv.at[side, side], where,
            ).start()

    @pl.loop(0, groups + 4)
    def _(t):
        @pl.when((t >= 2) & (t < groups + 2))
        def _():
            compute(t - 2)

        @pl.when((t >= 3) & (t < groups + 3))
        def _():
            combine(t - 3)

        @pl.when(t == groups + 2)
        def _():
            mix_start()

        @pl.when(t >= 4)
        def _():
            give_back(t - 4)

        @pl.when((t >= 1) & (t < groups + 1))
        def _():
            relay(t - 1)

        @pl.when(t < groups)
        def _():
            gather(t)

    mix_combine()
    for side in range(2):
        for half in range(2):
            block = mix_second.at[side, half]
            remote(
                block, block, mix_send.at[0], mix_second_recv.at[side, half], right
            ).wait_recv()
    for half in range(2):
        mixer_ref[half * half_rows : (half + 1) * half_rows, :] = (
            mix_partial[0, half].astype(F32)
            + mix_second[0, half].astype(F32)
            + mix_second[1, half].astype(F32)
        ).astype(BF16)

    for g in range(groups):
        for half in range(2):
            block = returned.at[g, half] if (g, half) != (last, 1) else returned.at[g, half, 0]
            remote(block, block, back_send.at[0], back_recv.at[g, half], right).wait_recv()

    for k in range(count):
        wide[k * chunk : (k + 1) * chunk, :] = returned[k // 4, (k // 2) % 2, k % 2].astype(F32)
    answers[used:slots, :] = jnp.zeros((slots - used, width), BF16)
    for strip in range(strips):
        answers[0:used, strip * LANES : (strip + 1) * LANES] = wide[
            pl.ds(strip, used, stride=strips), :
        ].astype(BF16)
    weights = jnp.concatenate(
        [picks[k : k + LANES, :].T for k in range(0, slots, LANES)], axis=1
    )
    high = weights.astype(BF16)
    low = (weights - high.astype(F32)).astype(BF16)
    for part in range(width // 256):
        columns = slice(part * 256, (part + 1) * 256)
        expert_ref[:, columns] = (
            dot(high, answers[:, columns]) + dot(low, answers[:, columns])
        ).astype(BF16)

    def left_all(amount, sem):
        block = summed.at[pl.ds(0, amount)]
        remote(block, block, sem, z_recv.at[0, 0], right).wait_send()

    left_all(count - 1, z_send.at[0])
    left_all(count - 1, back_send.at[0])
    for side in range(2):
        left_all(count, gather_send.at[side])
        for sem in (relay_send, first_send, direct_send, comb_send):
            left_all(count // 2, sem.at[side])
    for k in range(6):
        block = mix_first.at[0]
        remote(block, block, mix_send.at[k], z_recv.at[0, 0], right).wait_send()


def on_device(
    n_ep,
    n_tp,
    outer_gate,
    inner_gate,
    conv_input,
    conv_taps,
    mixer_weight,
    expert_input,
    norm_gain,
    expert_ids,
    route_weight,
    gate_weight,
    up_weight,
    down_weight,
):
    tokens, width = expert_input.shape
    top = expert_ids.shape[1]
    cap = 5 * tokens * top // (4 * n_ep)
    count = n_ep
    groups = n_ep // CORES // 2
    strips = width // LANES
    chunk = cap * strips
    slots = -(-count * cap // LANES) * LANES
    batch = 4 * 2 * CORES * cap
    length, channels = inner_gate.shape
    units = gate_weight.shape[2]
    vmem, dma = pltpu.VMEM, pltpu.SemaphoreType.DMA
    whole = pl.BlockSpec(memory_space=pltpu.VMEM)
    left_out = pl.BlockSpec(memory_space=pl.ANY)
    block = (groups, 2, CORES, chunk, LANES)
    call = pl.pallas_call(
        functools.partial(kernel, n_ep, n_tp, cap),
        out_shape=[jax.ShapeDtypeStruct((tokens, width), BF16)] * 2,
        in_specs=[whole] * 5 + [left_out] * 7,
        out_specs=[whole] * 2,
        scratch_shapes=[
            vmem((length, channels), BF16),
            vmem((length, channels), BF16),
            vmem((length, channels), BF16),
            vmem((channels, width), BF16),
            vmem((width, units), BF16),
            vmem((width, units), BF16),
            vmem((units, width), BF16),
            vmem((tokens, width), BF16),
            vmem((slots, tokens), F32),
            vmem((count * chunk, LANES), F32),
            vmem((count, chunk, LANES), BF16),
            vmem((groups, 4, 2, CORES, chunk, LANES), BF16),
            vmem((batch * strips, LANES), F32),
            vmem((batch, width), BF16),
            vmem((batch, units), BF16),
            vmem((groups, 4, 2, CORES, chunk, LANES), BF16),
            vmem(block, BF16),
            vmem((groups, 2, 2, CORES, chunk, LANES), BF16),
            vmem(block, BF16),
            vmem((count, chunk, LANES), BF16),
            vmem(block, BF16),
            vmem((slots, width), BF16),
            vmem((8, channels), F32),
            vmem((8, channels), F32),
            vmem((length + 8, channels), F32),
            vmem((4, 2, tokens // 2, width), BF16),
            vmem((2, tokens // 2, width), BF16),
            vmem((2, 2, tokens // 2, width), BF16),
            vmem((2, tokens // 2, width), BF16),
            dma((7,)),
            dma((1,)),
            dma((1,)),
            dma((1,)),
            dma((groups, 2)),
            dma((2,)),
            dma((groups, 2)),
            dma((2,)),
            dma((groups, 2)),
            dma((2,)),
            dma((groups, 2)),
            dma((2,)),
            dma((2,)),
            dma((groups, 2)),
            dma((1,)),
            dma((groups, 2)),
            dma((6,)),
            dma((2,)),
            dma((2, 2)),
        ],
        compiler_params=pltpu.CompilerParams(
            collective_id=0, has_side_effects=True, vmem_limit_bytes=60 * 1024 * 1024
        ),
        name="whole_step",
    )
    mixer_output, expert_output = call(
        expert_ids.T,
        route_weight.T,
        expert_input,
        norm_gain.reshape(1, width),
        conv_taps,
        outer_gate,
        inner_gate,
        conv_input,
        mixer_weight,
        gate_weight[0],
        up_weight[0],
        down_weight[0],
    )
    return mixer_output, expert_output


def solution(mesh):
    rows = P(("grp", "ep", "tp"), None)
    channels = P(("grp", "ep"), "tp")
    return jax.shard_map(
        functools.partial(on_device, mesh.shape["ep"], mesh.shape["tp"]),
        mesh=mesh,
        in_specs=(
            channels,
            channels,
            channels,
            P(None, "tp"),
            P("tp", None),
            rows,
            P(),
            rows,
            rows,
            P("ep", None, "tp"),
            P("ep", None, "tp"),
            P("ep", "tp", None),
        ),
        out_specs=(rows, rows),
        check_vma=False,
    )
```

```python
import functools

import jax
import jax.numpy as jnp
from jax import lax
from jax.experimental import pallas as pl
from jax.experimental.pallas import tpu as pltpu
from jax.sharding import PartitionSpec as P

TAPS = 3
CORES = 2
LANES = 128
EPSILON = 1e-06
MESH = pl.DeviceIdType.MESH
AHEAD = 2
MIX_AT = 1
F32 = jnp.float32
BF16 = jnp.bfloat16


def distances(n_z):
    far = n_z // 2
    rising = [d for d in range(4, far + 1) if d % 2 == far % 2]
    falling = [d for d in range(far, 1, -1) if d not in rising]
    return [1] + rising + falling


def offsets(n_z, g):
    d = distances(n_z)[g]
    return d, (n_z - d if d < n_z // 2 else 0)


def remote(source, target, send, recv, where):
    return pltpu.make_async_remote_copy(
        src_ref=source,
        dst_ref=target,
        send_sem=send,
        recv_sem=recv,
        device_id=where,
        device_id_type=MESH,
    )


def dot(a, b):
    return jnp.dot(a, b, preferred_element_type=F32)


def kernel(
    n_ep,
    n_tp,
    cap,
    ids_ref,
    route_ref,
    tokens_ref,
    gain_ref,
    taps_ref,
    outer_hbm,
    inner_hbm,
    conv_hbm,
    mixw_hbm,
    gate_hbm,
    up_hbm,
    down_hbm,
    mixer_ref,
    expert_ref,
    outer,
    inner,
    conv,
    mixw,
    gate_w,
    up_w,
    down_w,
    normed,
    picks,
    wide,
    outgoing,
    gathered,
    rows_f,
    rows_b,
    hidden,
    partial,
    first_in,
    second_in,
    combined,
    summed,
    returned,
    answers,
    tail_out,
    tail_in,
    gated,
    mix_partial,
    mix_first,
    mix_second,
    mix_combined,
    load_sem,
    halo_send,
    halo_recv,
    z_send,
    z_recv,
    gather_send,
    gather_recv,
    relay_send,
    relay_recv,
    first_send,
    first_recv,
    direct_send,
    comb_send,
    second_recv,
    back_send,
    back_recv,
    mix_send,
    mix_first_recv,
    mix_second_recv,
):
    n_z = n_ep // CORES
    groups = n_z // 2
    own = distances(n_z).index(groups)
    count = 2 * n_z
    tokens, width = tokens_ref.shape
    strips = width // LANES
    chunk = cap * strips
    slots = picks.shape[0]
    used = count * cap
    batch = 4 * 2 * CORES * cap

    me = lax.axis_index("ep")
    x = lax.axis_index("tp")
    z = me // CORES
    core = me % CORES
    right = {"tp": (x + 1) % n_tp}
    left = {"tp": (x + n_tp - 1) % n_tp}

    barrier = pltpu.get_barrier_semaphore()

    @pl.loop(1, n_ep)
    def _(k):
        pl.semaphore_signal(
            barrier, inc=1, device_id={"ep": (me + k) % n_ep}, device_id_type=MESH
        )

    pl.semaphore_signal(barrier, inc=1, device_id=right, device_id_type=MESH)
    pl.semaphore_signal(barrier, inc=1, device_id=left, device_id_type=MESH)

    loads = [
        pltpu.make_async_copy(source, target, load_sem.at[k])
        for k, (source, target) in enumerate(
            (
                (inner_hbm, inner),
                (conv_hbm, conv),
                (outer_hbm, outer),
                (mixw_hbm, mixw),
                (gate_hbm, gate_w),
                (up_hbm, up_w),
                (down_hbm, down_w),
            )
        )
    ]
    for load in loads:
        load.start()

    row = lax.broadcasted_iota(jnp.int32, (slots, tokens), 0)
    place = ((row.astype(F32) + 0.5) * (1.0 / cap)).astype(jnp.int32)
    slot = row - place * cap
    group_of = lax.shift_right_logical(place, 2)
    half_of = lax.shift_right_logical(place, 1) & 1
    offset = row * 0
    for g in range(groups):
        one, two = offsets(n_z, g)
        offset = jnp.where(group_of == g, jnp.where(half_of == 0, one, two), offset)
    target_z = z - offset
    target_z = jnp.where(target_z < 0, target_z + n_z, target_z)
    expert = jnp.where(row < used, target_z * CORES + (place & 1), -1)
    first_named = ids_ref[0:1, :] == expert
    second_named = ids_ref[1:2, :] == expert
    named = jnp.where(first_named, 1.0, 0.0) + jnp.where(second_named, 1.0, 0.0)
    before = lax.broadcasted_iota(jnp.int32, (tokens, tokens), 0) < lax.broadcasted_iota(
        jnp.int32, (tokens, tokens), 1
    )
    rank = dot(named.astype(BF16), jnp.where(before, 1.0, 0.0).astype(BF16))
    chosen = jnp.where(rank == slot.astype(F32), named, 0.0)
    weight = jnp.where(first_named, route_ref[0:1, :], 0.0) + jnp.where(
        second_named, route_ref[1:2, :], 0.0
    )
    picks[...] = chosen * weight

    values = tokens_ref[...].astype(F32)
    mean = jnp.mean(values * values, axis=1, keepdims=True)
    normed[...] = (values * lax.rsqrt(mean + EPSILON) * gain_ref[...]).astype(BF16)
    one_hot = chosen[0:used, :].astype(BF16)
    for pair in range(strips // 2):
        rows = dot(one_hot, normed[:, 2 * pair * LANES : 2 * (pair + 1) * LANES])
        wide[pl.ds(2 * pair, used, stride=strips), :] = rows[:, :LANES]
        wide[pl.ds(2 * pair + 1, used, stride=strips), :] = rows[:, LANES:]

    @pl.loop(0, count)
    def _(k):
        outgoing[k] = wide[pl.ds(pl.multiple_of(k * chunk, 16), chunk), :].astype(BF16)

    loads[0].wait()
    loads[1].wait()
    length = inner.shape[0]
    gated[pl.ds(8, length), :] = inner[...].astype(F32) * conv[...].astype(F32)
    tail_out[...] = gated[pl.ds(length, 8), :]

    pl.semaphore_wait(barrier, n_ep + 1)

    other = 1 - core

    def z_send_group(g):
        for half, offset in enumerate(offsets(n_z, g)):
            for to_core in range(CORES) if offset else (other,):
                remote(
                    outgoing.at[4 * g + 2 * half + to_core],
                    gathered.at[g, 0, half, core],
                    z_send.at[0],
                    z_recv.at[g, half],
                    {"ep": ((z + n_z - offset) % n_z) * CORES + to_core},
                ).start()

    halo = remote(
        tail_out, tail_in, halo_send.at[0], halo_recv.at[0], {"ep": (me + 1) % n_ep}
    )
    halo.start()
    for g in range(AHEAD):
        z_send_group(g)
    gathered[own, 0, 1, core] = outgoing[4 * own + 2 + core]

    for load in loads[2:4]:
        load.wait()
    halo.wait()
    gated[0:8, :] = jnp.where(me > 0, tail_in[...], 0.0)
    convolved = jnp.zeros((length, inner.shape[1]), F32)
    for tap in range(TAPS):
        convolved = convolved + taps_ref[tap : tap + 1, :] * gated[
            pl.ds(8 - (TAPS - 1) + tap, length), :
        ]
    inner[...] = (outer[...].astype(F32) * convolved).astype(BF16)
    half_rows = tokens // 2

    @pl.loop(0, n_tp * 2)
    def _(k):
        owner = (x + k // 2) % n_tp
        start = pl.multiple_of(owner * tokens + (k % 2) * half_rows, 16)
        mixed = inner[pl.ds(start, half_rows), :]
        for part in range(width // 512):
            columns = slice(part * 512, (part + 1) * 512)
            mix_partial[k // 2, k % 2, :, columns] = dot(mixed, mixw[:, columns]).astype(BF16)

    for load in loads[4:]:
        load.wait()

    def gather(g):
        block = gathered.at[g, 0, 0]
        remote(block, block, z_send.at[0], z_recv.at[g, 0], right).wait_recv()

        @pl.when(g != own)
        def _():
            block = gathered.at[g, 0, 1]
            remote(block, block, z_send.at[0], z_recv.at[g, 1], right).wait_recv()

        @pl.when(g == own)
        def _():
            block = gathered.at[g, 0, 1, 0]
            remote(block, block, z_send.at[0], z_recv.at[g, 1], right).wait_recv()

        for k in range(AHEAD, groups):

            @pl.when(g == k - AHEAD)
            def _():
                z_send_group(k)

        remote(
            gathered.at[g, 0], gathered.at[g, 3], gather_send.at[0], gather_recv.at[g, 0], right
        ).start()
        remote(
            gathered.at[g, 0], gathered.at[g, 1], gather_send.at[1], gather_recv.at[g, 1], left
        ).start()

    def relay(g):
        remote(
            gathered.at[g, 0], gathered.at[g, 3], gather_send.at[0], gather_recv.at[g, 0], right
        ).wait_recv()
        remote(
            gathered.at[g, 3, 0], gathered.at[g, 2, 0], relay_send.at[0], relay_recv.at[g, 0], right
        ).start()
        remote(
            gathered.at[g, 0], gathered.at[g, 1], gather_send.at[1], gather_recv.at[g, 1], left
        ).wait_recv()
        remote(
            gathered.at[g, 1, 1], gathered.at[g, 2, 1], relay_send.at[1], relay_recv.at[g, 1], left
        ).start()

    def compute(g):
        remote(
            gathered.at[g, 3, 0], gathered.at[g, 2, 0], relay_send.at[0], relay_recv.at[g, 0], right
        ).wait_recv()
        remote(
            gathered.at[g, 1, 1], gathered.at[g, 2, 1], relay_send.at[1], relay_recv.at[g, 1], left
        ).wait_recv()
        for k in range(batch // cap):
            rows_f[k * chunk : (k + 1) * chunk, :] = gathered[
                g, k // 4, (k // 2) % 2, k % 2
            ].astype(F32)
        for strip in range(strips):
            rows_b[:, strip * LANES : (strip + 1) * LANES] = rows_f[
                pl.ds(strip, batch, stride=strips), :
            ].astype(BF16)
        units = hidden.shape[1]
        step = min(256, units)
        for part in range(units // step):
            columns = slice(part * step, (part + 1) * step)
            gate = dot(rows_b[...], gate_w[:, columns])
            up = dot(rows_b[...], up_w[:, columns])
            hidden[:, columns] = (gate / (1.0 + jnp.exp(-gate)) * up).astype(BF16)
        for pair in range(strips // 2):
            rows = dot(hidden[...], down_w[:, 2 * pair * LANES : 2 * (pair + 1) * LANES])
            rows_f[pl.ds(2 * pair, batch, stride=strips), :] = rows[:, :LANES]
            rows_f[pl.ds(2 * pair + 1, batch, stride=strips), :] = rows[:, LANES:]
        for k in range(batch // cap):
            partial[g, k // 4, (k // 2) % 2, k % 2] = rows_f[
                k * chunk : (k + 1) * chunk, :
            ].astype(BF16)
        remote(
            partial.at[g, 2, 0], first_in.at[g, 0], first_send.at[0], first_recv.at[g, 0], right
        ).start()
        remote(
            partial.at[g, 2, 1], first_in.at[g, 1], first_send.at[1], first_recv.at[g, 1], left
        ).start()
        remote(
            partial.at[g, 1, 1], second_in.at[g, 0, 1], direct_send.at[0], second_recv.at[g, 0], right
        ).start()
        remote(
            partial.at[g, 3, 0], second_in.at[g, 1, 0], direct_send.at[1], second_recv.at[g, 1], left
        ).start()

    def combine(g):
        for side, slot, where in ((0, 1, right), (1, 3, left)):
            remote(
                partial.at[g, 2, side], first_in.at[g, side], first_send.at[side],
                first_recv.at[g, side], where,
            ).wait_recv()
            combined[g, side] = (
                partial[g, slot, side].astype(F32) + first_in[g, side].astype(F32)
            ).astype(BF16)
            remote(
                combined.at[g, side], second_in.at[g, side, side], comb_send.at[side],
                second_recv.at[g, side], where,
            ).start()

    def give_back(g):
        for side, where in ((0, right), (1, left)):
            block = second_in.at[g, side]
            remote(block, block, comb_send.at[side], second_recv.at[g, side], where).wait_recv()
        for half in range(2):
            for from_core in range(CORES):
                summed[4 * g + 2 * half + from_core] = (
                    partial[g, 0, half, from_core].astype(F32)
                    + second_in[g, 0, half, from_core].astype(F32)
                    + second_in[g, 1, half, from_core].astype(F32)
                ).astype(BF16)

        for k in range(groups):

            @pl.when(g == k)
            def _():
                for half, offset in enumerate(offsets(n_z, k)):
                    for to_core in range(CORES) if offset else (other,):
                        remote(
                            summed.at[4 * k + 2 * half + to_core],
                            returned.at[k, half, core],
                            back_send.at[0],
                            back_recv.at[k, half],
                            {"ep": ((z + offset) % n_z) * CORES + to_core},
                        ).start()

        @pl.when(g == own)
        def _():
            returned[own, 1, core] = summed[4 * own + 2 + core]

    def mix_start():
        remote(
            mix_partial.at[2, 0], mix_first.at[0], mix_send.at[0], mix_first_recv.at[0], right
        ).start()
        remote(
            mix_partial.at[2, 1], mix_first.at[1], mix_send.at[1], mix_first_recv.at[1], left
        ).start()
        remote(
            mix_partial.at[1, 1], mix_second.at[0, 1], mix_send.at[2], mix_second_recv.at[0, 1], right
        ).start()
        remote(
            mix_partial.at[3, 0], mix_second.at[1, 0], mix_send.at[3], mix_second_recv.at[1, 0], left
        ).start()

    def mix_combine():
        for side, slot, where in ((0, 1, right), (1, 3, left)):
            remote(
                mix_partial.at[2, side], mix_first.at[side], mix_send.at[side],
                mix_first_recv.at[side], where,
            ).wait_recv()
            mix_combined[side] = (
                mix_partial[slot, side].astype(F32) + mix_first[side].astype(F32)
            ).astype(BF16)
            remote(
                mix_combined.at[side], mix_second.at[side, side], mix_send.at[4 + side],
                mix_second_recv.at[side, side], where,
            ).start()

    @pl.loop(0, groups + 2)
    def _(t):
        @pl.when(t < groups)
        def _():
            gather(t)

        @pl.when(t == MIX_AT)
        def _():
            mix_start()

        @pl.when(t == MIX_AT + 1)
        def _():
            mix_combine()

        @pl.when((t >= 1) & (t < groups + 1))
        def _():
            compute(t - 1)

        @pl.when(t < groups)
        def _():
            relay(t)

        @pl.when(t >= 2)
        def _():
            give_back(t - 2)

        @pl.when((t >= 1) & (t < groups + 1))
        def _():
            combine(t - 1)

    for side in range(2):
        for half in range(2):
            block = mix_second.at[side, half]
            remote(
                block, block, mix_send.at[0], mix_second_recv.at[side, half], right
            ).wait_recv()
    for half in range(2):
        mixer_ref[half * half_rows : (half + 1) * half_rows, :] = (
            mix_partial[0, half].astype(F32)
            + mix_second[0, half].astype(F32)
            + mix_second[1, half].astype(F32)
        ).astype(BF16)

    for g in range(groups):
        for half in range(2):
            block = returned.at[g, half] if (g, half) != (own, 1) else returned.at[g, half, 0]
            remote(block, block, back_send.at[0], back_recv.at[g, half], right).wait_recv()

    for k in range(count):
        wide[k * chunk : (k + 1) * chunk, :] = returned[k // 4, (k // 2) % 2, k % 2].astype(F32)
    answers[used:slots, :] = jnp.zeros((slots - used, width), BF16)
    for strip in range(strips):
        answers[0:used, strip * LANES : (strip + 1) * LANES] = wide[
            pl.ds(strip, used, stride=strips), :
        ].astype(BF16)
    weights = jnp.concatenate(
        [picks[k : k + LANES, :].T for k in range(0, slots, LANES)], axis=1
    )
    high = weights.astype(BF16)
    low = (weights - high.astype(F32)).astype(BF16)
    for part in range(width // 256):
        columns = slice(part * 256, (part + 1) * 256)
        expert_ref[:, columns] = (
            dot(high, answers[:, columns]) + dot(low, answers[:, columns])
        ).astype(BF16)

    def left_all(amount, sem):
        block = summed.at[pl.ds(0, amount)]
        remote(block, block, sem, z_recv.at[0, 0], right).wait_send()

    left_all(count - 1, z_send.at[0])
    left_all(count - 1, back_send.at[0])
    for side in range(2):
        left_all(count, gather_send.at[side])
        for sem in (relay_send, first_send, direct_send, comb_send):
            left_all(count // 2, sem.at[side])
    for k in range(6):
        block = mix_first.at[0]
        remote(block, block, mix_send.at[k], z_recv.at[0, 0], right).wait_send()


def on_device(
    n_ep,
    n_tp,
    outer_gate,
    inner_gate,
    conv_input,
    conv_taps,
    mixer_weight,
    expert_input,
    norm_gain,
    expert_ids,
    route_weight,
    gate_weight,
    up_weight,
    down_weight,
):
    tokens, width = expert_input.shape
    top = expert_ids.shape[1]
    cap = 5 * tokens * top // (4 * n_ep)
    count = n_ep
    groups = n_ep // CORES // 2
    strips = width // LANES
    chunk = cap * strips
    slots = -(-count * cap // LANES) * LANES
    batch = 4 * 2 * CORES * cap
    length, channels = inner_gate.shape
    units = gate_weight.shape[2]
    vmem, dma = pltpu.VMEM, pltpu.SemaphoreType.DMA
    whole = pl.BlockSpec(memory_space=pltpu.VMEM)
    left_out = pl.BlockSpec(memory_space=pl.ANY)
    block = (groups, 2, CORES, chunk, LANES)
    call = pl.pallas_call(
        functools.partial(kernel, n_ep, n_tp, cap),
        out_shape=[jax.ShapeDtypeStruct((tokens, width), BF16)] * 2,
        in_specs=[whole] * 5 + [left_out] * 7,
        out_specs=[whole] * 2,
        scratch_shapes=[
            vmem((length, channels), BF16),
            vmem((length, channels), BF16),
            vmem((length, channels), BF16),
            vmem((channels, width), BF16),
            vmem((width, units), BF16),
            vmem((width, units), BF16),
            vmem((units, width), BF16),
            vmem((tokens, width), BF16),
            vmem((slots, tokens), F32),
            vmem((count * chunk, LANES), F32),
            vmem((count, chunk, LANES), BF16),
            vmem((groups, 4, 2, CORES, chunk, LANES), BF16),
            vmem((batch * strips, LANES), F32),
            vmem((batch, width), BF16),
            vmem((batch, units), BF16),
            vmem((groups, 4, 2, CORES, chunk, LANES), BF16),
            vmem(block, BF16),
            vmem((groups, 2, 2, CORES, chunk, LANES), BF16),
            vmem(block, BF16),
            vmem((count, chunk, LANES), BF16),
            vmem(block, BF16),
            vmem((slots, width), BF16),
            vmem((8, channels), F32),
            vmem((8, channels), F32),
            vmem((length + 8, channels), F32),
            vmem((4, 2, tokens // 2, width), BF16),
            vmem((2, tokens // 2, width), BF16),
            vmem((2, 2, tokens // 2, width), BF16),
            vmem((2, tokens // 2, width), BF16),
            dma((7,)),
            dma((1,)),
            dma((1,)),
            dma((1,)),
            dma((groups, 2)),
            dma((2,)),
            dma((groups, 2)),
            dma((2,)),
            dma((groups, 2)),
            dma((2,)),
            dma((groups, 2)),
            dma((2,)),
            dma((2,)),
            dma((groups, 2)),
            dma((1,)),
            dma((groups, 2)),
            dma((6,)),
            dma((2,)),
            dma((2, 2)),
        ],
        compiler_params=pltpu.CompilerParams(
            collective_id=0, has_side_effects=True, vmem_limit_bytes=60 * 1024 * 1024
        ),
        name="whole_step",
    )
    mixer_output, expert_output = call(
        expert_ids.T,
        route_weight.T,
        expert_input,
        norm_gain.reshape(1, width),
        conv_taps,
        outer_gate,
        inner_gate,
        conv_input,
        mixer_weight,
        gate_weight[0],
        up_weight[0],
        down_weight[0],
    )
    return mixer_output, expert_output


def solution(mesh):
    rows = P(("grp", "ep", "tp"), None)
    channels = P(("grp", "ep"), "tp")
    return jax.shard_map(
        functools.partial(on_device, mesh.shape["ep"], mesh.shape["tp"]),
        mesh=mesh,
        in_specs=(
            channels,
            channels,
            channels,
            P(None, "tp"),
            P("tp", None),
            rows,
            P(),
            rows,
            rows,
            P("ep", None, "tp"),
            P("ep", None, "tp"),
            P("ep", "tp", None),
        ),
        out_specs=(rows, rows),
        check_vma=False,
    )
```

```python
import functools

import jax
import jax.numpy as jnp
from jax import lax
from jax.experimental import pallas as pl
from jax.experimental.pallas import tpu as pltpu
from jax.sharding import PartitionSpec as P

TAPS = 3
CORES = 2
LANES = 128
EPSILON = 1e-06
MESH = pl.DeviceIdType.MESH
AHEAD = 3
FIRST = 2
GRANT = 58
PIECES = 4
F32 = jnp.float32
BF16 = jnp.bfloat16


def distances(n_z):
    far = n_z // 2
    rising = [d for d in range(4, far + 1) if d % 2 == far % 2]
    falling = [d for d in range(far, 1, -1) if d not in rising]
    return [1] + rising + falling


def offsets(n_z, g):
    d = distances(n_z)[g]
    return d, (n_z - d if d < n_z // 2 else 0)


def remote(source, target, send, recv, where):
    return pltpu.make_async_remote_copy(
        src_ref=source,
        dst_ref=target,
        send_sem=send,
        recv_sem=recv,
        device_id=where,
        device_id_type=MESH,
    )


def dot(a, b):
    return jnp.dot(a, b, preferred_element_type=F32)


def kernel(
    n_ep,
    n_tp,
    cap,
    ids_hbm,
    route_hbm,
    tokens_hbm,
    gain_hbm,
    taps_hbm,
    outer_hbm,
    inner_hbm,
    conv_hbm,
    mixw_hbm,
    gate_hbm,
    up_hbm,
    down_hbm,
    mixer_ref,
    expert_ref,
    ids_ref,
    route_ref,
    tokens_ref,
    gain_ref,
    taps_ref,
    outer,
    inner,
    conv,
    mixw,
    gate_w,
    up_w,
    down_w,
    normed,
    picks,
    wide,
    outgoing,
    gathered,
    rows_f,
    rows_b,
    hidden,
    partial,
    first_in,
    second_in,
    combined,
    summed,
    returned,
    answers,
    tail_out,
    tail_in,
    gated,
    mix_partial,
    mix_first,
    mix_second,
    mix_combined,
    total,
    small_sem,
    load_sem,
    halo_send,
    halo_recv,
    z_send,
    z_recv,
    gather_send,
    gather_recv,
    relay_send,
    relay_recv,
    first_send,
    first_recv,
    direct_send,
    comb_send,
    second_recv,
    back_send,
    back_recv,
    mix_send,
    mix_first_recv,
    mix_second_recv,
):
    n_z = n_ep // CORES
    groups = n_z // 2
    own = distances(n_z).index(groups)
    count = 2 * n_z
    tokens, width = tokens_ref.shape
    strips = width // LANES
    chunk = cap * strips
    slots = picks.shape[0]
    used = count * cap
    batch = 4 * 2 * CORES * cap

    me = lax.axis_index("ep")
    x = lax.axis_index("tp")
    z = me // CORES
    core = me % CORES
    right = {"tp": (x + 1) % n_tp}
    left = {"tp": (x + n_tp - 1) % n_tp}

    barrier = pltpu.get_barrier_semaphore()

    @pl.loop(1, n_ep)
    def _(k):
        pl.semaphore_signal(
            barrier, inc=1, device_id={"ep": (me + k) % n_ep}, device_id_type=MESH
        )

    pl.semaphore_signal(barrier, inc=1, device_id=right, device_id_type=MESH)
    pl.semaphore_signal(barrier, inc=1, device_id=left, device_id_type=MESH)

    smalls = [
        pltpu.make_async_copy(source, target, small_sem.at[k])
        for k, (source, target) in enumerate(
            (
                (ids_hbm, ids_ref),
                (route_hbm, route_ref),
                (tokens_hbm, tokens_ref),
                (gain_hbm, gain_ref),
                (taps_hbm, taps_ref),
            )
        )
    ]
    for small in smalls:
        small.start()
    loads = [
        pltpu.make_async_copy(source, target, load_sem.at[k])
        for k, (source, target) in enumerate(
            (
                (inner_hbm, inner),
                (conv_hbm, conv),
                (outer_hbm, outer),
                (mixw_hbm, mixw),
                (gate_hbm, gate_w),
                (up_hbm, up_w),
                (down_hbm, down_w),
            )
        )
    ]
    for load in loads:
        load.start()

    smalls[0].wait()
    smalls[1].wait()

    row = lax.broadcasted_iota(jnp.int32, (slots, tokens), 0)
    place = ((row.astype(F32) + 0.5) * (1.0 / cap)).astype(jnp.int32)
    slot = row - place * cap
    group_of = lax.shift_right_logical(place, 2)
    half_of = lax.shift_right_logical(place, 1) & 1
    offset = row * 0
    for g in range(groups):
        one, two = offsets(n_z, g)
        offset = jnp.where(group_of == g, jnp.where(half_of == 0, one, two), offset)
    target_z = z - offset
    target_z = jnp.where(target_z < 0, target_z + n_z, target_z)
    expert = jnp.where(row < used, target_z * CORES + (place & 1), -1)
    first_named = ids_ref[0:1, :] == expert
    second_named = ids_ref[1:2, :] == expert
    named = jnp.where(first_named, 1.0, 0.0) + jnp.where(second_named, 1.0, 0.0)
    before = lax.broadcasted_iota(jnp.int32, (tokens, tokens), 0) < lax.broadcasted_iota(
        jnp.int32, (tokens, tokens), 1
    )
    rank = dot(named.astype(BF16), jnp.where(before, 1.0, 0.0).astype(BF16))
    chosen = jnp.where(rank == slot.astype(F32), named, 0.0)
    weight = jnp.where(first_named, route_ref[0:1, :], 0.0) + jnp.where(
        second_named, route_ref[1:2, :], 0.0
    )
    picks[...] = chosen * weight

    for small in smalls[2:]:
        small.wait()
    values = tokens_ref[...].astype(F32)
    mean = jnp.mean(values * values, axis=1, keepdims=True)
    normed[...] = (values * lax.rsqrt(mean + EPSILON) * gain_ref[...]).astype(BF16)
    one_hot = chosen[0:used, :].astype(BF16)
    for pair in range(strips // 2):
        rows = dot(one_hot, normed[:, 2 * pair * LANES : 2 * (pair + 1) * LANES])
        wide[pl.ds(2 * pair, used, stride=strips), :] = rows[:, :LANES]
        wide[pl.ds(2 * pair + 1, used, stride=strips), :] = rows[:, LANES:]

    @pl.loop(0, count)
    def _(k):
        outgoing[k] = wide[pl.ds(pl.multiple_of(k * chunk, 16), chunk), :].astype(BF16)

    loads[0].wait()
    loads[1].wait()
    length = inner.shape[0]
    gated[pl.ds(8, length), :] = inner[...].astype(F32) * conv[...].astype(F32)
    tail_out[...] = gated[pl.ds(length, 8), :]

    pl.semaphore_wait(barrier, n_ep + 1)

    other = 1 - core

    def z_send_group(g):
        for half, offset in enumerate(offsets(n_z, g)):
            for to_core in range(CORES) if offset else (other,):
                remote(
                    outgoing.at[4 * g + 2 * half + to_core],
                    gathered.at[g, 0, half, core],
                    z_send.at[0],
                    z_recv.at[g, half],
                    {"ep": ((z + n_z - offset) % n_z) * CORES + to_core},
                ).start()

    halo = remote(
        tail_out, tail_in, halo_send.at[0], halo_recv.at[0], {"ep": (me + 1) % n_ep}
    )
    halo.start()
    for g in range(FIRST):
        z_send_group(g)
    gathered[own, 0, 1, core] = outgoing[4 * own + 2 + core]

    for load in loads[2:4]:
        load.wait()
    halo.wait()
    gated[0:8, :] = jnp.where(me > 0, tail_in[...], 0.0)
    convolved = jnp.zeros((length, inner.shape[1]), F32)
    for tap in range(TAPS):
        convolved = convolved + taps_ref[tap : tap + 1, :] * gated[
            pl.ds(8 - (TAPS - 1) + tap, length), :
        ]
    inner[...] = (outer[...].astype(F32) * convolved).astype(BF16)
    half_rows = tokens // 2

    @pl.loop(0, n_tp * 2)
    def _(k):
        owner = (x + k // 2) % n_tp
        start = pl.multiple_of(owner * tokens + (k % 2) * half_rows, 16)
        mixed = inner[pl.ds(start, half_rows), :]
        for part in range(width // 512):
            columns = slice(part * 512, (part + 1) * 512)
            mix_partial[k // 2, k % 2, :, columns] = dot(mixed, mixw[:, columns]).astype(BF16)

    for g in range(FIRST, min(AHEAD, groups)):
        z_send_group(g)
    for load in loads[4:]:
        load.wait()

    def gather(g):
        block = gathered.at[g, 0, 0]
        remote(block, block, z_send.at[0], z_recv.at[g, 0], right).wait_recv()

        @pl.when(g != own)
        def _():
            block = gathered.at[g, 0, 1]
            remote(block, block, z_send.at[0], z_recv.at[g, 1], right).wait_recv()

        @pl.when(g == own)
        def _():
            block = gathered.at[g, 0, 1, 0]
            remote(block, block, z_send.at[0], z_recv.at[g, 1], right).wait_recv()

        for k in range(AHEAD, groups):

            @pl.when(g == k - AHEAD)
            def _():
                z_send_group(k)

        remote(
            gathered.at[g, 0], gathered.at[g, 3], gather_send.at[0], gather_recv.at[g, 0], right
        ).start()
        remote(
            gathered.at[g, 0], gathered.at[g, 1], gather_send.at[1], gather_recv.at[g, 1], left
        ).start()

    def relay(g):
        remote(
            gathered.at[g, 0], gathered.at[g, 3], gather_send.at[0], gather_recv.at[g, 0], right
        ).wait_recv()
        remote(
            gathered.at[g, 3, 0], gathered.at[g, 2, 0], relay_send.at[0], relay_recv.at[g, 0], right
        ).start()
        remote(
            gathered.at[g, 0], gathered.at[g, 1], gather_send.at[1], gather_recv.at[g, 1], left
        ).wait_recv()
        remote(
            gathered.at[g, 1, 1], gathered.at[g, 2, 1], relay_send.at[1], relay_recv.at[g, 1], left
        ).start()

    def compute(g):
        remote(
            gathered.at[g, 3, 0], gathered.at[g, 2, 0], relay_send.at[0], relay_recv.at[g, 0], right
        ).wait_recv()
        remote(
            gathered.at[g, 1, 1], gathered.at[g, 2, 1], relay_send.at[1], relay_recv.at[g, 1], left
        ).wait_recv()
        for k in range(batch // cap):
            rows_f[k * chunk : (k + 1) * chunk, :] = gathered[
                g, k // 4, (k // 2) % 2, k % 2
            ].astype(F32)
        for strip in range(strips):
            rows_b[:, strip * LANES : (strip + 1) * LANES] = rows_f[
                pl.ds(strip, batch, stride=strips), :
            ].astype(BF16)
        units = hidden.shape[1]
        step = min(256, units)
        for part in range(units // step):
            columns = slice(part * step, (part + 1) * step)
            gate = dot(rows_b[...], gate_w[:, columns])
            up = dot(rows_b[...], up_w[:, columns])
            hidden[:, columns] = (gate / (1.0 + jnp.exp(-gate)) * up).astype(BF16)
        for pair in range(strips // 2):
            rows = dot(hidden[...], down_w[:, 2 * pair * LANES : 2 * (pair + 1) * LANES])
            rows_f[pl.ds(2 * pair, batch, stride=strips), :] = rows[:, :LANES]
            rows_f[pl.ds(2 * pair + 1, batch, stride=strips), :] = rows[:, LANES:]
        for k in range(batch // cap):
            partial[g, k // 4, (k // 2) % 2, k % 2] = rows_f[
                k * chunk : (k + 1) * chunk, :
            ].astype(BF16)
        remote(
            partial.at[g, 2, 0], first_in.at[g, 0], first_send.at[0], first_recv.at[g, 0], right
        ).start()
        remote(
            partial.at[g, 2, 1], first_in.at[g, 1], first_send.at[1], first_recv.at[g, 1], left
        ).start()
        remote(
            partial.at[g, 1, 1], second_in.at[g, 0, 1], direct_send.at[0], second_recv.at[g, 0], right
        ).start()
        remote(
            partial.at[g, 3, 0], second_in.at[g, 1, 0], direct_send.at[1], second_recv.at[g, 1], left
        ).start()

    def combine(g):
        for side, slot, where in ((0, 1, right), (1, 3, left)):
            remote(
                partial.at[g, 2, side], first_in.at[g, side], first_send.at[side],
                first_recv.at[g, side], where,
            ).wait_recv()
            combined[g, side] = (
                partial[g, slot, side].astype(F32) + first_in[g, side].astype(F32)
            ).astype(BF16)
            remote(
                combined.at[g, side], second_in.at[g, side, side], comb_send.at[side],
                second_recv.at[g, side], where,
            ).start()

    def give_back(g):
        for side, where in ((0, right), (1, left)):
            block = second_in.at[g, side]
            remote(block, block, comb_send.at[side], second_recv.at[g, side], where).wait_recv()
        for half in range(2):
            for from_core in range(CORES):
                summed[4 * g + 2 * half + from_core] = (
                    partial[g, 0, half, from_core].astype(F32)
                    + second_in[g, 0, half, from_core].astype(F32)
                    + second_in[g, 1, half, from_core].astype(F32)
                ).astype(BF16)

        for k in range(groups):

            @pl.when(g == k)
            def _():
                for half, offset in enumerate(offsets(n_z, k)):
                    for to_core in range(CORES) if offset else (other,):
                        remote(
                            summed.at[4 * k + 2 * half + to_core],
                            returned.at[k, half, core],
                            back_send.at[0],
                            back_recv.at[k, half],
                            {"ep": ((z + offset) % n_z) * CORES + to_core},
                        ).start()

        @pl.when(g == own)
        def _():
            returned[own, 1, core] = summed[4 * own + 2 + core]

    def mix_start():
        remote(
            mix_partial.at[2, 0], mix_first.at[0], mix_send.at[0], mix_first_recv.at[0], right
        ).start()
        remote(
            mix_partial.at[2, 1], mix_first.at[1], mix_send.at[1], mix_first_recv.at[1], left
        ).start()
        remote(
            mix_partial.at[1, 1], mix_second.at[0, 1], mix_send.at[2], mix_second_recv.at[0, 1], right
        ).start()
        remote(
            mix_partial.at[3, 0], mix_second.at[1, 0], mix_send.at[3], mix_second_recv.at[1, 0], left
        ).start()

    def mix_combine():
        for side, slot, where in ((0, 1, right), (1, 3, left)):
            remote(
                mix_partial.at[2, side], mix_first.at[side], mix_send.at[side],
                mix_first_recv.at[side], where,
            ).wait_recv()
            mix_combined[side] = (
                mix_partial[slot, side].astype(F32) + mix_first[side].astype(F32)
            ).astype(BF16)
            remote(
                mix_combined.at[side], mix_second.at[side, side], mix_send.at[4 + side],
                mix_second_recv.at[side, side], where,
            ).start()

    mix_start()

    @pl.loop(0, groups + 2)
    def _(t):
        @pl.when(t < groups)
        def _():
            gather(t)

        @pl.when((t >= 1) & (t < groups + 1))
        def _():
            compute(t - 1)

        @pl.when(t < groups)
        def _():
            relay(t)

        @pl.when(t >= 2)
        def _():
            give_back(t - 2)

        @pl.when((t >= 1) & (t < groups + 1))
        def _():
            combine(t - 1)

        @pl.when(t == groups - 1)
        def _():
            mix_combine()

    weights = jnp.concatenate(
        [picks[k : k + LANES, :].T for k in range(0, slots, LANES)], axis=1
    )
    high = weights.astype(BF16)
    low = (weights - high.astype(F32)).astype(BF16)
    answers[used:slots, :] = jnp.zeros((slots - used, width), BF16)

    def arrived(begin, end):
        for g in range(begin, end):
            for half in range(2):
                block = returned.at[g, half] if (g, half) != (own, 1) else returned.at[g, half, 0]
                remote(block, block, back_send.at[0], back_recv.at[g, half], right).wait_recv()
        start = 4 * begin * cap
        rows = 4 * (end - begin) * cap
        for k in range(4 * begin, 4 * end):
            wide[k * chunk : (k + 1) * chunk, :] = returned[k // 4, (k // 2) % 2, k % 2].astype(F32)
        for strip in range(strips):
            answers[start : start + rows, strip * LANES : (strip + 1) * LANES] = wide[
                pl.ds(start * strips + strip, rows, stride=strips), :
            ].astype(BF16)

    for side in range(2):
        for half in range(2):
            block = mix_second.at[side, half]
            remote(
                block, block, mix_send.at[0], mix_second_recv.at[side, half], right
            ).wait_recv()
    for half in range(2):
        mixer_ref[half * half_rows : (half + 1) * half_rows, :] = (
            mix_partial[0, half].astype(F32)
            + mix_second[0, half].astype(F32)
            + mix_second[1, half].astype(F32)
        ).astype(BF16)
    arrived(0, groups - 1)
    done = 4 * (groups - 1) * cap // LANES * LANES
    for part in range(width // 256):
        columns = slice(part * 256, (part + 1) * 256)
        rows = answers[0:done, columns]
        total[:, columns] = dot(high[:, 0:done], rows) + dot(low[:, 0:done], rows)
    arrived(groups - 1, groups)
    for part in range(width // 256):
        columns = slice(part * 256, (part + 1) * 256)
        rows = answers[done:slots, columns]
        expert_ref[:, columns] = (
            total[:, columns] + dot(high[:, done:slots], rows) + dot(low[:, done:slots], rows)
        ).astype(BF16)

    def left_all(amount, sem):
        block = summed.at[pl.ds(0, amount)]
        remote(block, block, sem, z_recv.at[0, 0], right).wait_send()

    left_all(count - 1, z_send.at[0])
    left_all(count - 1, back_send.at[0])
    for side in range(2):
        left_all(count, gather_send.at[side])
        for sem in (relay_send, first_send, direct_send, comb_send):
            left_all(count // 2, sem.at[side])
    for k in range(6):
        block = mix_first.at[0]
        remote(block, block, mix_send.at[k], z_recv.at[0, 0], right).wait_send()


def hand_on(one, two, one_out, two_out, held, in_sem, out_sem):
    rows = one.shape[0] // PIECES
    steps = []
    for k, (source, target) in enumerate(((one, one_out), (two, two_out))):
        for piece in range(PIECES):
            where = pl.ds(piece * rows, rows)
            place = held.at[k, where]
            steps.append(
                (
                    pltpu.make_async_copy(source.at[where], place, in_sem.at[k, piece]),
                    pltpu.make_async_copy(place, target.at[where], out_sem.at[k, piece]),
                )
            )
    for arrive, _ in steps:
        arrive.start()
    for arrive, leave in steps:
        arrive.wait()
        leave.start()
    for _, leave in steps:
        leave.wait()


def on_device(
    n_ep,
    n_tp,
    outer_gate,
    inner_gate,
    conv_input,
    conv_taps,
    mixer_weight,
    expert_input,
    norm_gain,
    expert_ids,
    route_weight,
    gate_weight,
    up_weight,
    down_weight,
):
    tokens, width = expert_input.shape
    top = expert_ids.shape[1]
    cap = 5 * tokens * top // (4 * n_ep)
    count = n_ep
    groups = n_ep // CORES // 2
    strips = width // LANES
    chunk = cap * strips
    slots = -(-count * cap // LANES) * LANES
    batch = 4 * 2 * CORES * cap
    length, channels = inner_gate.shape
    units = gate_weight.shape[2]
    vmem, dma = pltpu.VMEM, pltpu.SemaphoreType.DMA
    whole = pl.BlockSpec(memory_space=pltpu.VMEM)
    left_out = pl.BlockSpec(memory_space=pltpu.HBM)
    block = (groups, 2, CORES, chunk, LANES)
    call = pl.pallas_call(
        functools.partial(kernel, n_ep, n_tp, cap),
        out_shape=[jax.ShapeDtypeStruct((tokens, width), BF16)] * 2,
        in_specs=[left_out] * 12,
        out_specs=[whole] * 2,
        scratch_shapes=[
            vmem((top, tokens), jnp.int32),
            vmem((top, tokens), F32),
            vmem((tokens, width), BF16),
            vmem((1, width), F32),
            vmem((TAPS, channels), F32),
            vmem((length, channels), BF16),
            vmem((length, channels), BF16),
            vmem((length, channels), BF16),
            vmem((channels, width), BF16),
            vmem((width, units), BF16),
            vmem((width, units), BF16),
            vmem((units, width), BF16),
            vmem((tokens, width), BF16),
            vmem((slots, tokens), F32),
            vmem((count * chunk, LANES), F32),
            vmem((count, chunk, LANES), BF16),
            vmem((groups, 4, 2, CORES, chunk, LANES), BF16),
            vmem((batch * strips, LANES), F32),
            vmem((batch, width), BF16),
            vmem((batch, units), BF16),
            vmem((groups, 4, 2, CORES, chunk, LANES), BF16),
            vmem(block, BF16),
            vmem((groups, 2, 2, CORES, chunk, LANES), BF16),
            vmem(block, BF16),
            vmem((count, chunk, LANES), BF16),
            vmem(block, BF16),
            vmem((slots, width), BF16),
            vmem((8, channels), F32),
            vmem((8, channels), F32),
            vmem((length + 8, channels), F32),
            vmem((4, 2, tokens // 2, width), BF16),
            vmem((2, tokens // 2, width), BF16),
            vmem((2, 2, tokens // 2, width), BF16),
            vmem((2, tokens // 2, width), BF16),
            vmem((tokens, width), F32),
            dma((5,)),
            dma((7,)),
            dma((1,)),
            dma((1,)),
            dma((1,)),
            dma((groups, 2)),
            dma((2,)),
            dma((groups, 2)),
            dma((2,)),
            dma((groups, 2)),
            dma((2,)),
            dma((groups, 2)),
            dma((2,)),
            dma((2,)),
            dma((groups, 2)),
            dma((1,)),
            dma((groups, 2)),
            dma((6,)),
            dma((2,)),
            dma((2, 2)),
        ],
        compiler_params=pltpu.CompilerParams(
            collective_id=0, has_side_effects=True, vmem_limit_bytes=GRANT * 1024 * 1024
        ),
        name="whole_step",
    )
    mixer_output, expert_output = call(
        expert_ids.T,
        route_weight.T,
        expert_input,
        norm_gain.reshape(1, width),
        conv_taps,
        outer_gate,
        inner_gate,
        conv_input,
        mixer_weight,
        gate_weight[0],
        up_weight[0],
        down_weight[0],
    )
    return pl.pallas_call(
        hand_on,
        out_shape=[jax.ShapeDtypeStruct((tokens, width), BF16)] * 2,
        in_specs=[left_out] * 2,
        out_specs=[left_out] * 2,
        scratch_shapes=[
            vmem((2, tokens, width), BF16),
            dma((2, PIECES)),
            dma((2, PIECES)),
        ],
        compiler_params=pltpu.CompilerParams(vmem_limit_bytes=GRANT * 1024 * 1024),
        name="hand_on",
    )(mixer_output, expert_output)


def solution(mesh):
    rows = P(("grp", "ep", "tp"), None)
    channels = P(("grp", "ep"), "tp")
    return jax.shard_map(
        functools.partial(on_device, mesh.shape["ep"], mesh.shape["tp"]),
        mesh=mesh,
        in_specs=(
            channels,
            channels,
            channels,
            P(None, "tp"),
            P("tp", None),
            rows,
            P(),
            rows,
            rows,
            P("ep", None, "tp"),
            P("ep", None, "tp"),
            P("ep", "tp", None),
        ),
        out_specs=(rows, rows),
        check_vma=False,
    )
```

```python
import functools

import jax
import jax.numpy as jnp
from jax import lax
from jax.experimental import pallas as pl
from jax.experimental.pallas import tpu as pltpu
from jax.sharding import PartitionSpec as P

TAPS = 3
CORES = 2
LANES = 128
EPSILON = 1e-06
MESH = pl.DeviceIdType.MESH
AHEAD = 3
FIRST = 1
GRANT = 58
PIECES = 4
F32 = jnp.float32
BF16 = jnp.bfloat16


def distances(n_z):
    return [1] + list(range(n_z // 2, 1, -1))


def offsets(n_z, g):
    d = distances(n_z)[g]
    return d, (n_z - d if d < n_z // 2 else 0)


def remote(source, target, send, recv, where):
    return pltpu.make_async_remote_copy(
        src_ref=source,
        dst_ref=target,
        send_sem=send,
        recv_sem=recv,
        device_id=where,
        device_id_type=MESH,
    )


def dot(a, b):
    return jnp.dot(a, b, preferred_element_type=F32)


def kernel(
    n_ep,
    n_tp,
    cap,
    ids_hbm,
    route_hbm,
    tokens_hbm,
    gain_hbm,
    taps_hbm,
    outer_hbm,
    inner_hbm,
    conv_hbm,
    mixw_hbm,
    gate_hbm,
    up_hbm,
    down_hbm,
    mixer_ref,
    expert_ref,
    ids_ref,
    route_ref,
    tokens_ref,
    gain_ref,
    taps_ref,
    outer,
    inner,
    conv,
    mixw,
    gate_w,
    up_w,
    down_w,
    normed,
    picks,
    wide,
    outgoing,
    gathered,
    rows_f,
    rows_b,
    hidden,
    partial,
    first_in,
    second_in,
    combined,
    summed,
    returned,
    answers,
    tail_out,
    tail_in,
    gated,
    mix_partial,
    mix_first,
    mix_second,
    mix_combined,
    total,
    small_sem,
    load_sem,
    halo_send,
    halo_recv,
    z_send,
    z_recv,
    gather_send,
    gather_recv,
    relay_send,
    relay_recv,
    first_send,
    first_recv,
    direct_send,
    comb_send,
    second_recv,
    back_send,
    back_recv,
    mix_send,
    mix_first_recv,
    mix_second_recv,
):
    n_z = n_ep // CORES
    groups = n_z // 2
    own = distances(n_z).index(groups)
    count = 2 * n_z
    tokens, width = tokens_ref.shape
    strips = width // LANES
    chunk = cap * strips
    slots = picks.shape[0]
    used = count * cap
    batch = 4 * 2 * CORES * cap

    me = lax.axis_index("ep")
    x = lax.axis_index("tp")
    z = me // CORES
    core = me % CORES
    right = {"tp": (x + 1) % n_tp}
    left = {"tp": (x + n_tp - 1) % n_tp}

    barrier = pltpu.get_barrier_semaphore()

    @pl.loop(1, n_ep)
    def _(k):
        pl.semaphore_signal(
            barrier, inc=1, device_id={"ep": (me + k) % n_ep}, device_id_type=MESH
        )

    pl.semaphore_signal(barrier, inc=1, device_id=right, device_id_type=MESH)
    pl.semaphore_signal(barrier, inc=1, device_id=left, device_id_type=MESH)

    smalls = [
        pltpu.make_async_copy(source, target, small_sem.at[k])
        for k, (source, target) in enumerate(
            (
                (ids_hbm, ids_ref),
                (route_hbm, route_ref),
                (tokens_hbm, tokens_ref),
                (gain_hbm, gain_ref),
                (taps_hbm, taps_ref),
            )
        )
    ]
    for small in smalls:
        small.start()
    loads = [
        pltpu.make_async_copy(source, target, load_sem.at[k])
        for k, (source, target) in enumerate(
            (
                (inner_hbm, inner),
                (conv_hbm, conv),
                (outer_hbm, outer),
                (mixw_hbm, mixw),
                (gate_hbm, gate_w),
                (up_hbm, up_w),
                (down_hbm, down_w),
            )
        )
    ]
    for load in loads:
        load.start()

    smalls[0].wait()
    smalls[1].wait()

    row = lax.broadcasted_iota(jnp.int32, (slots, tokens), 0)
    place = ((row.astype(F32) + 0.5) * (1.0 / cap)).astype(jnp.int32)
    slot = row - place * cap
    group_of = lax.shift_right_logical(place, 2)
    half_of = lax.shift_right_logical(place, 1) & 1
    offset = row * 0
    for g in range(groups):
        one, two = offsets(n_z, g)
        offset = jnp.where(group_of == g, jnp.where(half_of == 0, one, two), offset)
    target_z = z - offset
    target_z = jnp.where(target_z < 0, target_z + n_z, target_z)
    expert = jnp.where(row < used, target_z * CORES + (place & 1), -1)
    first_named = ids_ref[0:1, :] == expert
    second_named = ids_ref[1:2, :] == expert
    named = jnp.where(first_named, 1.0, 0.0) + jnp.where(second_named, 1.0, 0.0)
    before = lax.broadcasted_iota(jnp.int32, (tokens, tokens), 0) < lax.broadcasted_iota(
        jnp.int32, (tokens, tokens), 1
    )
    rank = dot(named.astype(BF16), jnp.where(before, 1.0, 0.0).astype(BF16))
    chosen = jnp.where(rank == slot.astype(F32), named, 0.0)
    weight = jnp.where(first_named, route_ref[0:1, :], 0.0) + jnp.where(
        second_named, route_ref[1:2, :], 0.0
    )
    picks[...] = chosen * weight

    for small in smalls[2:]:
        small.wait()
    values = tokens_ref[...].astype(F32)
    mean = jnp.mean(values * values, axis=1, keepdims=True)
    normed[...] = (values * lax.rsqrt(mean + EPSILON) * gain_ref[...]).astype(BF16)
    one_hot = chosen[0:used, :].astype(BF16)
    for pair in range(strips // 2):
        rows = dot(one_hot, normed[:, 2 * pair * LANES : 2 * (pair + 1) * LANES])
        wide[pl.ds(2 * pair, used, stride=strips), :] = rows[:, :LANES]
        wide[pl.ds(2 * pair + 1, used, stride=strips), :] = rows[:, LANES:]

    @pl.loop(0, count)
    def _(k):
        outgoing[k] = wide[pl.ds(pl.multiple_of(k * chunk, 16), chunk), :].astype(BF16)

    loads[0].wait()
    loads[1].wait()
    length = inner.shape[0]
    gated[pl.ds(8, length), :] = inner[...].astype(F32) * conv[...].astype(F32)
    tail_out[...] = gated[pl.ds(length, 8), :]

    pl.semaphore_wait(barrier, n_ep + 1)

    other = 1 - core

    def z_send_group(g):
        for half, offset in enumerate(offsets(n_z, g)):
            for to_core in range(CORES) if offset else (other,):
                remote(
                    outgoing.at[4 * g + 2 * half + to_core],
                    gathered.at[g, 0, half, core],
                    z_send.at[0],
                    z_recv.at[g, half],
                    {"ep": ((z + n_z - offset) % n_z) * CORES + to_core},
                ).start()

    halo = remote(
        tail_out, tail_in, halo_send.at[0], halo_recv.at[0], {"ep": (me + 1) % n_ep}
    )
    halo.start()
    for g in range(FIRST):
        z_send_group(g)
    gathered[own, 0, 1, core] = outgoing[4 * own + 2 + core]

    for load in loads[2:4]:
        load.wait()
    halo.wait()
    gated[0:8, :] = jnp.where(me > 0, tail_in[...], 0.0)
    convolved = jnp.zeros((length, inner.shape[1]), F32)
    for tap in range(TAPS):
        convolved = convolved + taps_ref[tap : tap + 1, :] * gated[
            pl.ds(8 - (TAPS - 1) + tap, length), :
        ]
    inner[...] = (outer[...].astype(F32) * convolved).astype(BF16)
    half_rows = tokens // 2

    @pl.loop(0, n_tp * 2)
    def _(k):
        owner = (x + k // 2) % n_tp
        start = pl.multiple_of(owner * tokens + (k % 2) * half_rows, 16)
        mixed = inner[pl.ds(start, half_rows), :]
        for part in range(width // 512):
            columns = slice(part * 512, (part + 1) * 512)
            mix_partial[k // 2, k % 2, :, columns] = dot(mixed, mixw[:, columns]).astype(BF16)

    for g in range(FIRST, min(AHEAD, groups)):
        z_send_group(g)
    for load in loads[4:]:
        load.wait()

    def gather(g):
        block = gathered.at[g, 0, 0]
        remote(block, block, z_send.at[0], z_recv.at[g, 0], right).wait_recv()

        @pl.when(g != own)
        def _():
            block = gathered.at[g, 0, 1]
            remote(block, block, z_send.at[0], z_recv.at[g, 1], right).wait_recv()

        @pl.when(g == own)
        def _():
            block = gathered.at[g, 0, 1, 0]
            remote(block, block, z_send.at[0], z_recv.at[g, 1], right).wait_recv()

        for k in range(AHEAD, groups):

            @pl.when(g == k - AHEAD)
            def _():
                z_send_group(k)

        remote(
            gathered.at[g, 0], gathered.at[g, 3], gather_send.at[0], gather_recv.at[g, 0], right
        ).start()
        remote(
            gathered.at[g, 0], gathered.at[g, 1], gather_send.at[1], gather_recv.at[g, 1], left
        ).start()

    def relay(g):
        remote(
            gathered.at[g, 0], gathered.at[g, 3], gather_send.at[0], gather_recv.at[g, 0], right
        ).wait_recv()
        remote(
            gathered.at[g, 3, 0], gathered.at[g, 2, 0], relay_send.at[0], relay_recv.at[g, 0], right
        ).start()
        remote(
            gathered.at[g, 0], gathered.at[g, 1], gather_send.at[1], gather_recv.at[g, 1], left
        ).wait_recv()
        remote(
            gathered.at[g, 1, 1], gathered.at[g, 2, 1], relay_send.at[1], relay_recv.at[g, 1], left
        ).start()

    def compute(g):
        remote(
            gathered.at[g, 3, 0], gathered.at[g, 2, 0], relay_send.at[0], relay_recv.at[g, 0], right
        ).wait_recv()
        remote(
            gathered.at[g, 1, 1], gathered.at[g, 2, 1], relay_send.at[1], relay_recv.at[g, 1], left
        ).wait_recv()
        for k in range(batch // cap):
            rows_f[k * chunk : (k + 1) * chunk, :] = gathered[
                g, k // 4, (k // 2) % 2, k % 2
            ].astype(F32)
        for strip in range(strips):
            rows_b[:, strip * LANES : (strip + 1) * LANES] = rows_f[
                pl.ds(strip, batch, stride=strips), :
            ].astype(BF16)
        units = hidden.shape[1]
        step = min(256, units)
        for part in range(units // step):
            columns = slice(part * step, (part + 1) * step)
            gate = dot(rows_b[...], gate_w[:, columns])
            up = dot(rows_b[...], up_w[:, columns])
            hidden[:, columns] = (gate / (1.0 + jnp.exp(-gate)) * up).astype(BF16)
        for pair in range(strips // 2):
            rows = dot(hidden[...], down_w[:, 2 * pair * LANES : 2 * (pair + 1) * LANES])
            rows_f[pl.ds(2 * pair, batch, stride=strips), :] = rows[:, :LANES]
            rows_f[pl.ds(2 * pair + 1, batch, stride=strips), :] = rows[:, LANES:]
        for k in range(batch // cap):
            partial[g, k // 4, (k // 2) % 2, k % 2] = rows_f[
                k * chunk : (k + 1) * chunk, :
            ].astype(BF16)
        remote(
            partial.at[g, 2, 0], first_in.at[g, 0], first_send.at[0], first_recv.at[g, 0], right
        ).start()
        remote(
            partial.at[g, 2, 1], first_in.at[g, 1], first_send.at[1], first_recv.at[g, 1], left
        ).start()
        remote(
            partial.at[g, 1, 1], second_in.at[g, 0, 1], direct_send.at[0], second_recv.at[g, 0], right
        ).start()
        remote(
            partial.at[g, 3, 0], second_in.at[g, 1, 0], direct_send.at[1], second_recv.at[g, 1], left
        ).start()

    def combine(g):
        for side, slot, where in ((0, 1, right), (1, 3, left)):
            remote(
                partial.at[g, 2, side], first_in.at[g, side], first_send.at[side],
                first_recv.at[g, side], where,
            ).wait_recv()
            combined[g, side] = (
                partial[g, slot, side].astype(F32) + first_in[g, side].astype(F32)
            ).astype(BF16)
            remote(
                combined.at[g, side], second_in.at[g, side, side], comb_send.at[side],
                second_recv.at[g, side], where,
            ).start()

    def give_back(g):
        for side, where in ((0, right), (1, left)):
            block = second_in.at[g, side]
            remote(block, block, comb_send.at[side], second_recv.at[g, side], where).wait_recv()
        for half in range(2):
            for from_core in range(CORES):
                summed[4 * g + 2 * half + from_core] = (
                    partial[g, 0, half, from_core].astype(F32)
                    + second_in[g, 0, half, from_core].astype(F32)
                    + second_in[g, 1, half, from_core].astype(F32)
                ).astype(BF16)

        for k in range(groups):

            @pl.when(g == k)
            def _():
                for half, offset in enumerate(offsets(n_z, k)):
                    for to_core in range(CORES) if offset else (other,):
                        remote(
                            summed.at[4 * k + 2 * half + to_core],
                            returned.at[k, half, core],
                            back_send.at[0],
                            back_recv.at[k, half],
                            {"ep": ((z + offset) % n_z) * CORES + to_core},
                        ).start()

        @pl.when(g == own)
        def _():
            returned[own, 1, core] = summed[4 * own + 2 + core]

    def mix_start():
        remote(
            mix_partial.at[2, 0], mix_first.at[0], mix_send.at[0], mix_first_recv.at[0], right
        ).start()
        remote(
            mix_partial.at[2, 1], mix_first.at[1], mix_send.at[1], mix_first_recv.at[1], left
        ).start()
        remote(
            mix_partial.at[1, 1], mix_second.at[0, 1], mix_send.at[2], mix_second_recv.at[0, 1], right
        ).start()
        remote(
            mix_partial.at[3, 0], mix_second.at[1, 0], mix_send.at[3], mix_second_recv.at[1, 0], left
        ).start()

    def mix_combine():
        for side, slot, where in ((0, 1, right), (1, 3, left)):
            remote(
                mix_partial.at[2, side], mix_first.at[side], mix_send.at[side],
                mix_first_recv.at[side], where,
            ).wait_recv()
            mix_combined[side] = (
                mix_partial[slot, side].astype(F32) + mix_first[side].astype(F32)
            ).astype(BF16)
            remote(
                mix_combined.at[side], mix_second.at[side, side], mix_send.at[4 + side],
                mix_second_recv.at[side, side], where,
            ).start()

    mix_start()

    @pl.loop(0, groups + 2)
    def _(t):
        @pl.when(t < groups)
        def _():
            gather(t)

        @pl.when((t >= 1) & (t < groups + 1))
        def _():
            compute(t - 1)

        @pl.when(t < groups)
        def _():
            relay(t)

        @pl.when(t >= 2)
        def _():
            give_back(t - 2)

        @pl.when((t >= 1) & (t < groups + 1))
        def _():
            combine(t - 1)

        @pl.when(t == groups - 1)
        def _():
            mix_combine()

    weights = jnp.concatenate(
        [picks[k : k + LANES, :].T for k in range(0, slots, LANES)], axis=1
    )
    high = weights.astype(BF16)
    low = (weights - high.astype(F32)).astype(BF16)
    answers[used:slots, :] = jnp.zeros((slots - used, width), BF16)

    def arrived(begin, end):
        for g in range(begin, end):
            for half in range(2):
                block = returned.at[g, half] if (g, half) != (own, 1) else returned.at[g, half, 0]
                remote(block, block, back_send.at[0], back_recv.at[g, half], right).wait_recv()
        start = 4 * begin * cap
        rows = 4 * (end - begin) * cap
        for k in range(4 * begin, 4 * end):
            wide[k * chunk : (k + 1) * chunk, :] = returned[k // 4, (k // 2) % 2, k % 2].astype(F32)
        for strip in range(strips):
            answers[start : start + rows, strip * LANES : (strip + 1) * LANES] = wide[
                pl.ds(start * strips + strip, rows, stride=strips), :
            ].astype(BF16)

    for side in range(2):
        for half in range(2):
            block = mix_second.at[side, half]
            remote(
                block, block, mix_send.at[0], mix_second_recv.at[side, half], right
            ).wait_recv()
    for half in range(2):
        mixer_ref[half * half_rows : (half + 1) * half_rows, :] = (
            mix_partial[0, half].astype(F32)
            + mix_second[0, half].astype(F32)
            + mix_second[1, half].astype(F32)
        ).astype(BF16)
    arrived(0, groups - 1)
    done = 4 * (groups - 1) * cap // LANES * LANES
    for part in range(width // 256):
        columns = slice(part * 256, (part + 1) * 256)
        rows = answers[0:done, columns]
        total[:, columns] = dot(high[:, 0:done], rows) + dot(low[:, 0:done], rows)
    arrived(groups - 1, groups)
    for part in range(width // 256):
        columns = slice(part * 256, (part + 1) * 256)
        rows = answers[done:slots, columns]
        expert_ref[:, columns] = (
            total[:, columns] + dot(high[:, done:slots], rows) + dot(low[:, done:slots], rows)
        ).astype(BF16)

    def left_all(amount, sem):
        block = summed.at[pl.ds(0, amount)]
        remote(block, block, sem, z_recv.at[0, 0], right).wait_send()

    left_all(count - 1, z_send.at[0])
    left_all(count - 1, back_send.at[0])
    for side in range(2):
        left_all(count, gather_send.at[side])
        for sem in (relay_send, first_send, direct_send, comb_send):
            left_all(count // 2, sem.at[side])
    for k in range(6):
        block = mix_first.at[0]
        remote(block, block, mix_send.at[k], z_recv.at[0, 0], right).wait_send()


def hand_on(one, two, one_out, two_out, held, in_sem, out_sem):
    rows = one.shape[0] // PIECES
    steps = []
    for k, (source, target) in enumerate(((one, one_out), (two, two_out))):
        for piece in range(PIECES):
            where = pl.ds(piece * rows, rows)
            place = held.at[k, where]
            steps.append(
                (
                    pltpu.make_async_copy(source.at[where], place, in_sem.at[k, piece]),
                    pltpu.make_async_copy(place, target.at[where], out_sem.at[k, piece]),
                )
            )
    for arrive, _ in steps:
        arrive.start()
    for arrive, leave in steps:
        arrive.wait()
        leave.start()
    for _, leave in steps:
        leave.wait()


def on_device(
    n_ep,
    n_tp,
    outer_gate,
    inner_gate,
    conv_input,
    conv_taps,
    mixer_weight,
    expert_input,
    norm_gain,
    expert_ids,
    route_weight,
    gate_weight,
    up_weight,
    down_weight,
):
    tokens, width = expert_input.shape
    top = expert_ids.shape[1]
    cap = 5 * tokens * top // (4 * n_ep)
    count = n_ep
    groups = n_ep // CORES // 2
    strips = width // LANES
    chunk = cap * strips
    slots = -(-count * cap // LANES) * LANES
    batch = 4 * 2 * CORES * cap
    length, channels = inner_gate.shape
    units = gate_weight.shape[2]
    vmem, dma = pltpu.VMEM, pltpu.SemaphoreType.DMA
    whole = pl.BlockSpec(memory_space=pltpu.VMEM)
    left_out = pl.BlockSpec(memory_space=pltpu.HBM)
    block = (groups, 2, CORES, chunk, LANES)
    call = pl.pallas_call(
        functools.partial(kernel, n_ep, n_tp, cap),
        out_shape=[jax.ShapeDtypeStruct((tokens, width), BF16)] * 2,
        in_specs=[left_out] * 12,
        out_specs=[whole] * 2,
        scratch_shapes=[
            vmem((top, tokens), jnp.int32),
            vmem((top, tokens), F32),
            vmem((tokens, width), BF16),
            vmem((1, width), F32),
            vmem((TAPS, channels), F32),
            vmem((length, channels), BF16),
            vmem((length, channels), BF16),
            vmem((length, channels), BF16),
            vmem((channels, width), BF16),
            vmem((width, units), BF16),
            vmem((width, units), BF16),
            vmem((units, width), BF16),
            vmem((tokens, width), BF16),
            vmem((slots, tokens), F32),
            vmem((count * chunk, LANES), F32),
            vmem((count, chunk, LANES), BF16),
            vmem((groups, 4, 2, CORES, chunk, LANES), BF16),
            vmem((batch * strips, LANES), F32),
            vmem((batch, width), BF16),
            vmem((batch, units), BF16),
            vmem((groups, 4, 2, CORES, chunk, LANES), BF16),
            vmem(block, BF16),
            vmem((groups, 2, 2, CORES, chunk, LANES), BF16),
            vmem(block, BF16),
            vmem((count, chunk, LANES), BF16),
            vmem(block, BF16),
            vmem((slots, width), BF16),
            vmem((8, channels), F32),
            vmem((8, channels), F32),
            vmem((length + 8, channels), F32),
            vmem((4, 2, tokens // 2, width), BF16),
            vmem((2, tokens // 2, width), BF16),
            vmem((2, 2, tokens // 2, width), BF16),
            vmem((2, tokens // 2, width), BF16),
            vmem((tokens, width), F32),
            dma((5,)),
            dma((7,)),
            dma((1,)),
            dma((1,)),
            dma((1,)),
            dma((groups, 2)),
            dma((2,)),
            dma((groups, 2)),
            dma((2,)),
            dma((groups, 2)),
            dma((2,)),
            dma((groups, 2)),
            dma((2,)),
            dma((2,)),
            dma((groups, 2)),
            dma((1,)),
            dma((groups, 2)),
            dma((6,)),
            dma((2,)),
            dma((2, 2)),
        ],
        compiler_params=pltpu.CompilerParams(
            collective_id=0, has_side_effects=True, vmem_limit_bytes=GRANT * 1024 * 1024
        ),
        name="whole_step",
    )
    mixer_output, expert_output = call(
        expert_ids.T,
        route_weight.T,
        expert_input,
        norm_gain.reshape(1, width),
        conv_taps,
        outer_gate,
        inner_gate,
        conv_input,
        mixer_weight,
        gate_weight[0],
        up_weight[0],
        down_weight[0],
    )
    return pl.pallas_call(
        hand_on,
        out_shape=[jax.ShapeDtypeStruct((tokens, width), BF16)] * 2,
        in_specs=[left_out] * 2,
        out_specs=[left_out] * 2,
        scratch_shapes=[
            vmem((2, tokens, width), BF16),
            dma((2, PIECES)),
            dma((2, PIECES)),
        ],
        compiler_params=pltpu.CompilerParams(vmem_limit_bytes=GRANT * 1024 * 1024),
        name="hand_on",
    )(mixer_output, expert_output)


def solution(mesh):
    rows = P(("grp", "ep", "tp"), None)
    channels = P(("grp", "ep"), "tp")
    return jax.shard_map(
        functools.partial(on_device, mesh.shape["ep"], mesh.shape["tp"]),
        mesh=mesh,
        in_specs=(
            channels,
            channels,
            channels,
            P(None, "tp"),
            P("tp", None),
            rows,
            P(),
            rows,
            rows,
            P("ep", None, "tp"),
            P("ep", None, "tp"),
            P("ep", "tp", None),
        ),
        out_specs=(rows, rows),
        check_vma=False,
    )
```
